32 devices in a mesh: st: 4 (over y, x), tp: 8 (over z, core).
Axes of the slice: x: 2, y: 2, z: 4, core: 2. Of those that a mesh axis runs over, the one named last changes fastest.
Arguments:
- normed: bfloat16 [2048, 2048], P('st'), may hold values from -128 to 128
- store: bfloat16 [8192, 2048], P('st'), may hold values from -5 to 5
- passage_ids: int32 [16, 2], P('st'), may hold values from 0 to 127, as said below
- w_query: bfloat16 [2048, 2048], P(None, 'tp'), as said below
- w_gate: bfloat16 [2048, 2048], P(None, 'tp'), may hold values from -0.125 to 0.125
- w_key: bfloat16 [2048, 2048], P(None, 'tp'), as said below
- w_value: bfloat16 [2048, 2048], P(None, 'tp'), may hold values from -0.125 to 0.125
- cotangent: bfloat16 [2048, 2048], P('st', 'tp'), may hold values from -6 to 6
Outputs:
- grad_rows: float32 [2048, 2048], P('st', 'tp')
- grad_store: float32 [8192, 2048], P('st', 'tp')
- grad_query_weight: float32 [2048, 2048], P('st', 'tp')
The draws below stay inside these ranges and needn't reach their ends.
Inputs may be any that keep to these rules, and one draw needn't show every extreme that they name: `passage_ids`: each row names 2 passages. The passages read by the blocks of one index of st are all different, and at most 4 of them belong to any one owner (the owner of passage p is the index p // 32 of st). In every draw some owner has one of its passages read by every index of st. `w_query`: entries lie within 6 * 2048 ** -0.5 in magnitude. `w_key`: entries lie within 8 * 2048 ** -0.5 in magnitude.
All inputs are finite; a program needn't handle non-finite values.
Results may differ from the reference program's by a relative error of at most 0.019.
Values may be sent and summed in bfloat16 or wider, within the bound.
A program may use at most 128 MiB of HBM per device.

```python
import jax
import jax.numpy as jnp
from jax import lax

D = 2048
DH = 128
BLK = 128
R = 2
PLEN = 64
TOK_DEV = 512
PASS_DEV = 32
TOKENS = 2048
NPASS = 128
STORE_ROWS = 8192


def request_table(key):
    base = jax.random.fold_in(key, 11)
    owners_count = NPASS // PASS_DEV
    requests = TOK_DEV // BLK * R
    slot_most = max(1, 2 * requests // owners_count)
    slot_count = owners_count * slot_most
    subkeys = jax.random.split(base, 5)
    popular = jax.random.randint(subkeys[0], (owners_count,), 0, 2)
    hottest = jax.random.randint(subkeys[1], (), 0, owners_count)
    device = jnp.arange(owners_count, dtype=jnp.int32)[:, None]
    slot_ids = jnp.arange(slot_count, dtype=jnp.int32)[None, :]
    slot_owner = slot_ids // slot_most
    slot_rank = slot_ids % slot_most
    previous = (device - 1) % owners_count
    opposite = (device + owners_count // 2) % owners_count
    forced = ((slot_owner == hottest) | (slot_owner == previous)).astype(jnp.int32)
    halfway = ((slot_owner == opposite) & (slot_rank == 0)).astype(jnp.int32)
    leading = ((slot_owner == previous) & (slot_rank == 0)).astype(jnp.int32)
    tier = popular[slot_owner] + 3 * forced + 2 * halfway + 8 * leading
    noise = jax.random.randint(subkeys[2], (owners_count, slot_count), 0, 65536)
    score = (tier * 65536 + noise) * slot_count + slot_ids
    chosen = jnp.argsort(-score, axis=1)[:, :requests]
    chosen_owner = chosen // slot_most
    picks = jax.random.randint(subkeys[3], (owners_count, owners_count), 0, PASS_DEV)
    picks = picks.at[0, owners_count - 1].set(PASS_DEV - 1)
    picks = picks.at[1 % owners_count, 0].set(0)
    first_pick = jnp.take_along_axis(picks, chosen_owner, axis=1)
    local_ids = (first_pick + chosen % slot_most) % PASS_DEV
    passage = chosen_owner * PASS_DEV + local_ids
    shuffle = jax.random.randint(subkeys[4], (owners_count, requests), 0, 1 << 20) * requests
    shuffle = shuffle + jnp.arange(requests, dtype=jnp.int32)[None, :]
    arrangement = jnp.argsort(shuffle, axis=1)
    passage = jnp.take_along_axis(passage, arrangement, axis=1)
    return passage.reshape(-1, R).astype(jnp.int32)


def store_values(key):
    return jnp.clip(jax.random.normal(jax.random.fold_in(key, 21), (STORE_ROWS, D), jnp.float32), -5.0, 5.0)


def query_weight(key):
    fresh = jax.random.normal(jax.random.fold_in(key, 31), (D, D), jnp.float32)
    return jnp.clip(fresh, -6.0, 6.0) * D ** (-0.5)


def draw_passage_ids(key, part):
    return request_table(key)


def draw_store(key, part):
    return store_values(key).astype(jnp.bfloat16)


def draw_w_query(key, part):
    return query_weight(key).astype(jnp.bfloat16)


def draw_w_key(key, part):
    fresh = jnp.clip(jax.random.normal(jax.random.fold_in(key, 41), (D, D), jnp.float32), -6.0, 6.0) * D ** (-0.5)
    return fresh.astype(jnp.bfloat16)


def draw_normed(key, part):
    rows = jnp.clip(jax.random.normal(jax.random.fold_in(key, 51), (TOKENS, D), jnp.float32), -6.0, 6.0)
    return rows.astype(jnp.bfloat16)


def level_of(own_key, dims, pieces, low, largest):
    gain = 1.0
    for axis_at, parts in pieces:
        heights = jax.random.uniform(jax.random.fold_in(jax.random.fold_in(own_key, 6), axis_at), (parts,), jnp.float32, low / len(pieces), largest / len(pieces))
        gain = gain * jnp.repeat(jnp.exp(heights), dims[axis_at] // parts).reshape((-1,) + (1,) * (len(dims) - 1 - axis_at))
    return gain


def bell_draw(stream_key, dims, scale, bound, shards=(), kind=jnp.bfloat16):
    entries = jax.random.normal(stream_key, dims, jnp.float32) * scale
    if len(shards) > 0:
        entries = level_of(stream_key, dims, shards, -0.22, 0.18) * entries
    return jnp.clip(entries, min=-bound, max=bound).astype(kind)


def setup_inputs(seed: int = 0) -> dict:
    seeds = jax.random.split(jax.random.key(seed), 9)
    normed = draw_normed(jax.random.fold_in(seeds[8], 71), 0)
    store = draw_store(jax.random.fold_in(seeds[8], 71), 0)
    passage_ids = draw_passage_ids(jax.random.fold_in(seeds[8], 71), 0)
    w_query = draw_w_query(jax.random.fold_in(seeds[8], 71), 0)
    w_gate = bell_draw(seeds[4], (D, D), D ** -0.5, 0.125, ((1, 8),))
    w_key = draw_w_key(jax.random.fold_in(seeds[8], 71), 0)
    w_value = bell_draw(seeds[6], (D, D), D ** -0.5, 0.125, ((1, 8),))
    cotangent = bell_draw(seeds[7], (TOKENS, D), 1.0, 6.0, ((0, 4), (1, 8)))
    return dict(normed=normed, store=store, passage_ids=passage_ids, w_query=w_query, w_gate=w_gate, w_key=w_key, w_value=w_value, cotangent=cotangent)


def reference(normed, store, passage_ids, w_query, w_gate, w_key, w_value, cotangent):
    tokens, model_width = normed.shape
    blocks = tokens // BLK
    heads = model_width // DH
    score_scale = DH ** -0.5
    queries = jnp.dot(normed, w_query, preferred_element_type=jnp.float32).astype(jnp.bfloat16)
    gate_open = jax.nn.sigmoid(jnp.dot(normed, w_gate, preferred_element_type=jnp.float32))
    key_all = jnp.dot(store, w_key, preferred_element_type=jnp.float32).astype(jnp.bfloat16)
    value_all = jnp.dot(store, w_value, preferred_element_type=jnp.float32).astype(jnp.bfloat16)
    key_all = key_all.reshape(NPASS, PLEN, heads, DH)
    value_all = value_all.reshape(NPASS, PLEN, heads, DH)
    flat_ids = passage_ids.reshape(-1).astype(jnp.int32)
    key_rows = jnp.take(key_all, flat_ids, axis=0).reshape(blocks, R * PLEN, heads, DH).astype(jnp.float32)
    value_rows = jnp.take(value_all, flat_ids, axis=0).reshape(blocks, R * PLEN, heads, DH).astype(jnp.float32)
    q_blocks = queries.reshape(blocks, BLK, heads, DH).astype(jnp.float32)
    scores = jnp.einsum("bthd,bshd->bhts", q_blocks, key_rows) * score_scale
    attn_probs = jax.nn.softmax(scores, axis=-1)
    probs_low = attn_probs.astype(jnp.bfloat16).astype(jnp.float32)
    attended = jnp.einsum("bhts,bshd->bthd", probs_low, value_rows)
    gate_blocks = gate_open.reshape(blocks, BLK, heads, DH)
    upstream = cotangent.astype(jnp.float32).reshape(blocks, BLK, heads, DH)
    d_attended = (upstream * gate_blocks).astype(jnp.bfloat16).astype(jnp.float32)
    d_gate = (upstream * attended * gate_blocks * (1.0 - gate_blocks)).astype(jnp.bfloat16)
    d_values = jnp.einsum("bhts,bthd->bshd", probs_low, d_attended).astype(jnp.bfloat16)
    d_probs = jnp.einsum("bthd,bshd->bhts", d_attended, value_rows)
    row_delta = jnp.sum(d_probs * attn_probs, axis=-1, keepdims=True)
    d_scores = (attn_probs * (d_probs - row_delta) * score_scale).astype(jnp.bfloat16).astype(jnp.float32)
    d_query = jnp.einsum("bhts,bshd->bthd", d_scores, key_rows).astype(jnp.bfloat16).reshape(tokens, model_width)
    d_keys = jnp.einsum("bhts,bthd->bshd", d_scores, q_blocks).astype(jnp.bfloat16)
    grad_rows = jnp.dot(d_query, w_query.T, preferred_element_type=jnp.float32)
    grad_rows = grad_rows + jnp.dot(d_gate.reshape(tokens, model_width), w_gate.T, preferred_element_type=jnp.float32)
    reads_keys = d_keys.reshape(blocks * R, PLEN, model_width).astype(jnp.float32)
    reads_values = d_values.reshape(blocks * R, PLEN, model_width).astype(jnp.float32)
    summed_keys = jnp.zeros((NPASS, PLEN, model_width), jnp.float32).at[flat_ids].add(reads_keys)
    summed_values = jnp.zeros((NPASS, PLEN, model_width), jnp.float32).at[flat_ids].add(reads_values)
    grad_store = jnp.dot(summed_keys.reshape(NPASS * PLEN, model_width), w_key.astype(jnp.float32).T,
                         precision=lax.Precision.HIGHEST)
    grad_store = grad_store + jnp.dot(summed_values.reshape(NPASS * PLEN, model_width),
                                      w_value.astype(jnp.float32).T, precision=lax.Precision.HIGHEST)
    grad_query_weight = jnp.dot(normed.T, d_query, preferred_element_type=jnp.float32)
    return grad_rows, grad_store, grad_query_weight
```

```python
import functools

import jax
import jax.numpy as jnp
from jax import lax
from jax.experimental import pallas as pl
from jax.experimental.pallas import tpu as pltpu
from jax.sharding import PartitionSpec as P

DH = 128
BLK = 128
PLEN = 64
GROUP = 4
CORES = 2
F32 = jnp.float32
BF16 = jnp.bfloat16
MESH = pl.DeviceIdType.MESH


def dot_nn(a, b):
    return lax.dot_general(a, b, (((1,), (0,)), ((), ())), preferred_element_type=F32)


def dot_nt(a, b):
    return lax.dot_general(a, b, (((1,), (1,)), ((), ())), preferred_element_type=F32)


def dot_tn(a, b):
    return lax.dot_general(a, b, (((0,), (0,)), ((), ())), preferred_element_type=F32)


def rows_at(index, size):
    return pl.ds(pl.multiple_of(index * size, size), size)


def project_kernel(ids, *refs):
    passages = refs[:GROUP]
    wk_ref, wv_ref, out_ref = refs[GROUP:]
    rows = jnp.concatenate([p[...] for p in passages], axis=0)
    width = wk_ref.shape[1]
    out_ref[:, :width] = dot_nn(rows, wk_ref[...]).astype(BF16)
    out_ref[:, width:] = dot_nn(rows, wv_ref[...]).astype(BF16)


def project(store, ids, w_key, w_value):
    slots = ids.shape[0]
    depth, width = w_key.shape
    passage = lambda g: pl.BlockSpec((PLEN, depth), lambda i, ids: (ids[GROUP * i + g], 0))
    weight = pl.BlockSpec((depth, width), lambda i, ids: (0, 0))
    return pl.pallas_call(
        project_kernel,
        out_shape=jax.ShapeDtypeStruct((slots * PLEN, 2 * width), BF16),
        grid_spec=pltpu.PrefetchScalarGridSpec(
            num_scalar_prefetch=1,
            grid=(slots // GROUP,),
            in_specs=[passage(g) for g in range(GROUP)] + [weight, weight],
            out_specs=pl.BlockSpec((GROUP * PLEN, 2 * width), lambda i, ids: (i, 0)),
        ),
        compiler_params=pltpu.CompilerParams(vmem_limit_bytes=32 << 20),
        name="project",
    )(ids, *([store] * GROUP), w_key, w_value)


def main_kernel(
    st_n, tp_n, reads,
    slot_of, req_of, served, normed, w_q, w_g, w_k, w_v, cot,
    rows_out, ret_out, gqw_out,
    arrived, q_s, gate_s, dq_s, dg_s, dp_s,
    x_out, x_in, z_out, z_in, own, part, r_out, r_in, g_out, g_in, g_own,
    kv_ss, kv_rs, x_ss, x_rs, z_ss, z_rs, r_ss, r_rs, g_ss, g_rs,
):
    me_st, me_tp = lax.axis_index("st"), lax.axis_index("tp")
    z_n = tp_n // CORES
    me_z, me_c = me_tp // CORES, me_tp % CORES
    mate = (me_st, me_z * CORES + 1 - me_c)
    tok, hw = cot.shape
    depth = w_q.shape[0]
    heads = hw // DH
    blocks = tok // BLK
    cw = depth // tp_n
    slots = served.shape[0] // st_n
    scale = DH ** (-0.5)

    def st_peer(d):
        return lax.rem(me_st + d, st_n)

    def st_from(d):
        return lax.rem(me_st + st_n - d, st_n)

    def z_peer(d):
        return lax.rem(me_z + d, z_n)

    barrier = pltpu.get_barrier_semaphore()
    for d in range(1, st_n):
        pl.semaphore_signal(barrier, inc=1, device_id=(st_peer(d), me_tp), device_id_type=MESH)
    for d in range(1, z_n):
        pl.semaphore_signal(
            barrier, inc=1, device_id=(me_st, z_peer(d) * CORES + me_c), device_id_type=MESH
        )
    pl.semaphore_signal(barrier, inc=1, device_id=mate, device_id_type=MESH)
    pl.semaphore_wait(barrier, st_n + z_n - 1)

    def remote(src, dst, ss, rs, dev):
        return pltpu.make_async_remote_copy(
            src_ref=src, dst_ref=dst, send_sem=ss, recv_sem=rs, device_id=dev, device_id_type=MESH
        )

    sends = []

    def go(copy):
        copy.start()
        sends.append(copy)

    for d in range(1, st_n):
        go(remote(
            served.at[rows_at(st_peer(d), slots)], arrived.at[rows_at(me_st, slots)],
            kv_ss.at[d], kv_rs.at[d], (st_peer(d), me_tp),
        ))
    arrived[rows_at(me_st, slots)] = served[rows_at(me_st, slots)]

    tile = 2 * BLK

    @pl.loop(0, tok // tile)
    def _(i):
        span = rows_at(i, tile)
        q_s[span, :] = dot_nn(normed[span, :], w_q[...]).astype(BF16)
        gate_s[span, :] = jax.nn.sigmoid(dot_nn(normed[span, :], w_g[...]))

    for d in range(1, st_n):
        here = arrived.at[rows_at(st_from(d), slots)]
        remote(here, here, kv_ss.at[d], kv_rs.at[d], (st_peer(d), me_tp)).wait_recv()

    for b in range(blocks):
        kv = jnp.concatenate(
            [arrived[slot_of[b * reads + r]] for r in range(reads)], axis=0
        )
        toks = slice(b * BLK, (b + 1) * BLK)
        span = reads * PLEN
        ctx = slice(b * span, (b + 1) * span)
        for h in range(heads):
            ch = slice(h * DH, (h + 1) * DH)
            chv = slice(hw + h * DH, hw + (h + 1) * DH)
            k, v = kv[:, ch], kv[:, chv]
            q = q_s[toks, ch]
            gate = gate_s[toks, ch]
            up = cot[toks, ch].astype(F32)
            s = dot_nt(q, k) * scale
            e = jnp.exp(s - jnp.max(s, axis=1, keepdims=True))
            p = e / jnp.sum(e, axis=1, keepdims=True)
            low = p.astype(BF16)
            att = dot_nn(low, v)
            d_att = (up * gate).astype(BF16)
            dg_s[toks, ch] = (up * att * gate * (1.0 - gate)).astype(BF16)
            dp_s[ctx, chv] = dot_tn(low, d_att).astype(BF16)
            d_p = dot_nt(d_att, v)
            delta = jnp.sum(d_p * p, axis=1, keepdims=True)
            d_s = (p * (d_p - delta) * scale).astype(BF16)
            dq_s[toks, ch] = dot_nn(d_s, k).astype(BF16)
            dp_s[ctx, ch] = dot_tn(d_s, q).astype(BF16)

    def chunk(which, t):
        w_rows = rows_at(t, cw)
        if which == 0:
            return dot_nt(dp_s[:, :hw], w_k[w_rows, :]) + dot_nt(dp_s[:, hw:], w_v[w_rows, :])
        return dot_nt(dq_s[...], w_q[w_rows, :]) + dot_nt(dg_s[...], w_g[w_rows, :])

    order = list(range(1, z_n)) + [0]

    def mate_stage(which):
        for d in order:
            n = which * z_n + d
            x_out[n] = chunk(which, z_peer(d) * CORES + 1 - me_c).astype(BF16)
            go(remote(x_out.at[n], x_in.at[n], x_ss.at[n], x_rs.at[n], mate))

    def chip_stage(which):
        for d in order:
            n = which * z_n + d
            mine = chunk(which, z_peer(d) * CORES + me_c)
            remote(x_in.at[n], x_in.at[n], x_ss.at[n], x_rs.at[n], mate).wait_recv()
            total = mine + x_in[n].astype(F32)
            if d == 0:
                own[which] = total
            else:
                z_out[n] = total.astype(BF16)
                go(remote(
                    z_out.at[n], z_in.at[n], z_ss.at[n], z_rs.at[n],
                    (me_st, z_peer(d) * CORES + me_c),
                ))

    def gathered(which):
        total = own[which]
        for d in range(1, z_n):
            n = which * z_n + d
            remote(
                z_in.at[n], z_in.at[n], z_ss.at[n], z_rs.at[n],
                (me_st, z_peer(d) * CORES + me_c),
            ).wait_recv()
            total = total + z_in[n].astype(F32)
        return total

    mate_stage(0)
    chip_stage(0)
    mate_stage(1)
    chip_stage(1)

    dw = depth // st_n
    for d in list(range(1, st_n)) + [0]:
        term = dot_tn(normed[:, rows_at(st_peer(d), dw)], dq_s[...])
        if d == 0:
            g_own[...] = term
        else:
            g_out[d] = term.astype(BF16)
            go(remote(
                g_out.at[d], g_in.at[d], g_ss.at[d], g_rs.at[d], (st_peer(d), me_tp)
            ))

    part[...] = gathered(0).astype(BF16).reshape(part.shape)
    for s in range(st_n * slots):
        r_out[s] = part[req_of[s]]
    for d in range(1, st_n):
        go(remote(
            r_out.at[rows_at(st_peer(d), slots)], r_in.at[rows_at(me_st, slots)],
            r_ss.at[d], r_rs.at[d], (st_peer(d), me_tp),
        ))
    ret_out[rows_at(me_st, slots)] = r_out[rows_at(me_st, slots)]

    total = g_own[...]
    for d in range(1, st_n):
        remote(g_in.at[d], g_in.at[d], g_ss.at[d], g_rs.at[d], (st_peer(d), me_tp)).wait_recv()
        total = total + g_in[d].astype(F32)
    gqw_out[...] = total

    for d in range(1, st_n):
        span = rows_at(st_from(d), slots)
        remote(
            r_in.at[span], r_in.at[span], r_ss.at[d], r_rs.at[d], (st_peer(d), me_tp)
        ).wait_recv()
        ret_out[span] = r_in[span]

    rows_out[...] = gathered(1)
    for copy in sends:
        copy.wait_send()


def main_call(st_n, tp_n, reads, slot_of, req_of, served, normed, w_q, w_g, w_k, w_v, cot):
    tok, hw = cot.shape
    depth = w_q.shape[0]
    cw, dw, z_n = depth // tp_n, depth // st_n, tp_n // CORES
    ctx = tok // BLK * reads * PLEN
    slot_total = served.shape[0]
    vmem = pl.BlockSpec(memory_space=pltpu.VMEM)
    smem = pl.BlockSpec(memory_space=pltpu.SMEM)
    piece = lambda rows, n=2 * z_n: pltpu.VMEM((n, rows, cw), BF16)
    sem = lambda n: pltpu.SemaphoreType.DMA((n,))
    rows_most = max(ctx, tok)
    assert ctx == tok
    return pl.pallas_call(
        functools.partial(main_kernel, st_n, tp_n, reads),
        out_shape=(
            jax.ShapeDtypeStruct((tok, cw), F32),
            jax.ShapeDtypeStruct((slot_total, PLEN, cw), BF16),
            jax.ShapeDtypeStruct((dw, hw), F32),
        ),
        in_specs=[smem, smem] + [vmem] * 7,
        out_specs=(vmem, vmem, vmem),
        scratch_shapes=[
            pltpu.VMEM((slot_total, PLEN, 2 * hw), BF16),
            pltpu.VMEM((tok, hw), BF16),
            pltpu.VMEM((tok, hw), F32),
            pltpu.VMEM((tok, hw), BF16),
            pltpu.VMEM((tok, hw), BF16),
            pltpu.VMEM((ctx, 2 * hw), BF16),
            piece(rows_most), piece(rows_most), piece(rows_most), piece(rows_most),
            pltpu.VMEM((2, rows_most, cw), F32),
            pltpu.VMEM((ctx // PLEN, PLEN, cw), BF16),
            pltpu.VMEM((slot_total, PLEN, cw), BF16),
            pltpu.VMEM((slot_total, PLEN, cw), BF16),
            pltpu.VMEM((st_n, dw, hw), BF16),
            pltpu.VMEM((st_n, dw, hw), BF16),
            pltpu.VMEM((dw, hw), F32),
            sem(st_n), sem(st_n), sem(2 * z_n), sem(2 * z_n), sem(2 * z_n), sem(2 * z_n),
            sem(st_n), sem(st_n), sem(st_n), sem(st_n),
        ],
        compiler_params=pltpu.CompilerParams(
            collective_id=0, has_side_effects=True, vmem_limit_bytes=56 << 20
        ),
        name="main",
    )(slot_of, req_of, served, normed, w_q, w_g, w_k, w_v, cot)


def spread_kernel(ids, returned, out_ref):
    out_ref[...] = jnp.zeros_like(out_ref)
    for s in range(ids.shape[0]):
        passage = ids[s]

        @pl.when(passage >= 0)
        def _():
            span = rows_at(passage, PLEN)
            out_ref[span, :] += returned[s].astype(F32)


def spread(ids, returned, rows):
    return pl.pallas_call(
        spread_kernel,
        out_shape=jax.ShapeDtypeStruct((rows, returned.shape[2]), F32),
        in_specs=[
            pl.BlockSpec(memory_space=pltpu.SMEM),
            pl.BlockSpec(memory_space=pltpu.VMEM),
        ],
        out_specs=pl.BlockSpec(memory_space=pltpu.VMEM),
        compiler_params=pltpu.CompilerParams(vmem_limit_bytes=16 << 20),
        name="spread",
    )(ids, returned)


def shards(normed, store, passage_ids, w_query, w_gate, w_key, w_value, cotangent):
    peer_count = lax.axis_size("st")
    blocks, read_count = passage_ids.shape
    requests = blocks * read_count
    slot_most = max(1, 2 * requests // peer_count)
    slot_count = peer_count * slot_most
    pass_dev = store.shape[0] // PLEN
    flat_ids = passage_ids.reshape(requests)
    owners = flat_ids // pass_dev
    local_ids = flat_ids % pass_dev
    positions = jnp.arange(requests, dtype=jnp.int32)
    before = (owners[:, None] == owners[None, :]) & (positions[None, :] < positions[:, None])
    slot_of = owners * slot_most + jnp.sum(before.astype(jnp.int32), axis=1)
    slot_hit = slot_of[:, None] == jnp.arange(slot_count, dtype=jnp.int32)[None, :]
    slot_table = jnp.max(jnp.where(slot_hit, local_ids[:, None], -1), axis=0)
    req_of = jnp.max(jnp.where(slot_hit, positions[:, None], 0), axis=0)
    served_ids = lax.all_to_all(
        slot_table.reshape(peer_count, slot_most), "st", split_axis=0, concat_axis=0, tiled=True
    ).reshape(slot_count)
    served = project(store, jnp.maximum(served_ids, 0), w_key, w_value)
    served = served.reshape(slot_count, PLEN, served.shape[1])
    grad_rows, returned, grad_query_weight = main_call(
        peer_count, lax.axis_size("tp"), read_count,
        slot_of, req_of, served, normed, w_query, w_gate, w_key, w_value, cotangent,
    )
    grad_store = spread(served_ids, returned, store.shape[0])
    return (grad_rows, grad_store, grad_query_weight)


def solution(mesh):
    placed = (
        P("st", None),
        P("st", None),
        P("st", None),
        P(None, "tp"),
        P(None, "tp"),
        P(None, "tp"),
        P(None, "tp"),
        P("st", "tp"),
    )
    return jax.shard_map(
        shards,
        mesh=mesh,
        in_specs=placed,
        out_specs=(P("st", "tp"), P("st", "tp"), P("st", "tp")),
        check_vma=False,
    )
```

```python
import functools

import jax
import jax.numpy as jnp
from jax import lax
from jax.experimental import pallas as pl
from jax.experimental.pallas import tpu as pltpu
from jax.sharding import PartitionSpec as P

DH = 128
BLK = 128
PLEN = 64
GROUP = 4
CORES = 2
F32 = jnp.float32
BF16 = jnp.bfloat16
MESH = pl.DeviceIdType.MESH


def dot_nn(a, b):
    return lax.dot_general(a, b, (((1,), (0,)), ((), ())), preferred_element_type=F32)


def dot_nt(a, b):
    return lax.dot_general(a, b, (((1,), (1,)), ((), ())), preferred_element_type=F32)


def dot_tn(a, b):
    return lax.dot_general(a, b, (((0,), (0,)), ((), ())), preferred_element_type=F32)


def rows_at(index, size):
    return pl.ds(pl.multiple_of(index * size, size), size)


def project_kernel(ids, *refs):
    passages = refs[:GROUP]
    wk_ref, wv_ref, out_ref = refs[GROUP:]
    rows = jnp.concatenate([p[...] for p in passages], axis=0)
    width = wk_ref.shape[1]
    out_ref[:, :width] = dot_nn(rows, wk_ref[...]).astype(BF16)
    out_ref[:, width:] = dot_nn(rows, wv_ref[...]).astype(BF16)


def project(store, ids, w_key, w_value):
    slots = ids.shape[0]
    depth, width = w_key.shape
    passage = lambda g: pl.BlockSpec((PLEN, depth), lambda i, ids: (ids[GROUP * i + g], 0))
    weight = pl.BlockSpec((depth, width), lambda i, ids: (0, 0))
    return pl.pallas_call(
        project_kernel,
        out_shape=jax.ShapeDtypeStruct((slots * PLEN, 2 * width), BF16),
        grid_spec=pltpu.PrefetchScalarGridSpec(
            num_scalar_prefetch=1,
            grid=(slots // GROUP,),
            in_specs=[passage(g) for g in range(GROUP)] + [weight, weight],
            out_specs=pl.BlockSpec((GROUP * PLEN, 2 * width), lambda i, ids: (i, 0)),
        ),
        compiler_params=pltpu.CompilerParams(vmem_limit_bytes=58 << 20),
        name="project",
    )(ids, *([store] * GROUP), w_key, w_value)


def main_kernel(
    st_n, tp_n, reads,
    slot_of, req_of, served, normed, w_q, w_g, w_k, w_v, cot,
    rows_out, ret_out, gqw_out,
    arrived, q_s, gate_s, dq_s, dg_s, dp_s,
    x_out, x_in, z_out, up_in, dn_in, own, part, r_out, r_in, g_out, g_in, g_own,
    kv_ss, kv_rs, x_ss, x_rs, z_ss, up_rs, dn_rs, r_ss, r_rs, g_ss, g_rs,
):
    me_st, me_tp = lax.axis_index("st"), lax.axis_index("tp")
    z_n = tp_n // CORES
    me_z, me_c = me_tp // CORES, me_tp % CORES
    mate = (me_st, me_z * CORES + 1 - me_c)
    tok, hw = cot.shape
    depth = w_q.shape[0]
    heads = hw // DH
    blocks = tok // BLK
    cw = depth // tp_n
    slots = served.shape[0] // st_n
    scale = DH ** (-0.5)

    def st_peer(d):
        return lax.rem(me_st + d, st_n)

    def st_from(d):
        return lax.rem(me_st + st_n - d, st_n)

    def z_peer(d):
        return lax.rem(me_z + d, z_n)

    barrier = pltpu.get_barrier_semaphore()
    for d in range(1, st_n):
        pl.semaphore_signal(barrier, inc=1, device_id=(st_peer(d), me_tp), device_id_type=MESH)
    for d in range(1, z_n):
        pl.semaphore_signal(
            barrier, inc=1, device_id=(me_st, z_peer(d) * CORES + me_c), device_id_type=MESH
        )
    pl.semaphore_signal(barrier, inc=1, device_id=mate, device_id_type=MESH)
    pl.semaphore_wait(barrier, st_n + z_n - 1)

    def remote(src, dst, ss, rs, dev):
        return pltpu.make_async_remote_copy(
            src_ref=src, dst_ref=dst, send_sem=ss, recv_sem=rs, device_id=dev, device_id_type=MESH
        )

    sends = []

    def go(copy):
        copy.start()
        sends.append(copy)

    for d in range(1, st_n):
        go(remote(
            served.at[rows_at(st_peer(d), slots)], arrived.at[rows_at(me_st, slots)],
            kv_ss.at[d], kv_rs.at[d], (st_peer(d), me_tp),
        ))
    arrived[rows_at(me_st, slots)] = served[rows_at(me_st, slots)]

    tile = 2 * BLK

    @pl.loop(0, tok // tile)
    def _(i):
        span = rows_at(i, tile)
        q_s[span, :] = dot_nn(normed[span, :], w_q[...]).astype(BF16)
        gate_s[span, :] = jax.nn.sigmoid(dot_nn(normed[span, :], w_g[...]))

    for d in range(1, st_n):
        here = arrived.at[rows_at(st_from(d), slots)]
        remote(here, here, kv_ss.at[d], kv_rs.at[d], (st_peer(d), me_tp)).wait_recv()

    for b in range(blocks):
        kv = jnp.concatenate(
            [arrived[slot_of[b * reads + r]] for r in range(reads)], axis=0
        )
        toks = slice(b * BLK, (b + 1) * BLK)
        span = reads * PLEN
        ctx = slice(b * span, (b + 1) * span)
        for h in range(heads):
            ch = slice(h * DH, (h + 1) * DH)
            chv = slice(hw + h * DH, hw + (h + 1) * DH)
            k, v = kv[:, ch], kv[:, chv]
            q = q_s[toks, ch]
            gate = gate_s[toks, ch]
            up = cot[toks, ch].astype(F32)
            s = dot_nt(q, k) * scale
            e = jnp.exp(s - jnp.max(s, axis=1, keepdims=True))
            p = e / jnp.sum(e, axis=1, keepdims=True)
            low = p.astype(BF16)
            att = dot_nn(low, v)
            d_att = (up * gate).astype(BF16)
            dg_s[toks, ch] = (up * att * gate * (1.0 - gate)).astype(BF16)
            dp_s[ctx, chv] = dot_tn(low, d_att).astype(BF16)
            d_p = dot_nt(d_att, v)
            delta = jnp.sum(d_p * p, axis=1, keepdims=True)
            d_s = (p * (d_p - delta) * scale).astype(BF16)
            dq_s[toks, ch] = dot_nn(d_s, k).astype(BF16)
            dp_s[ctx, ch] = dot_tn(d_s, q).astype(BF16)

    def chunk(which, t):
        w_rows = rows_at(t, cw)
        if which == 0:
            return dot_nt(dp_s[:, :hw], w_k[w_rows, :]) + dot_nt(dp_s[:, hw:], w_v[w_rows, :])
        return dot_nt(dq_s[...], w_q[w_rows, :]) + dot_nt(dg_s[...], w_g[w_rows, :])

    order = []
    for i in range((z_n + 1) // 2):
        order += [z_n - 1 - i, i] if z_n - 1 - i != i else [i]
    above, below = me_z < z_n - 1, me_z > 0

    def mate_stage(which):
        for t in order:
            n = which * z_n + t
            x_out[n] = chunk(which, t * CORES + 1 - me_c).astype(BF16)
            go(remote(x_out.at[n], x_in.at[n], x_ss.at[n], x_rs.at[n], mate))

    def hop(n, up):
        landing, rs = (up_in, up_rs) if up else (dn_in, dn_rs)
        to = me_z + 1 if up else me_z - 1
        return remote(
            z_out.at[n], landing.at[n], z_ss.at[n], rs.at[n], (me_st, to * CORES + me_c)
        )

    def chip_stage(which):
        for t in order:
            n = which * z_n + t
            mine = chunk(which, t * CORES + me_c)
            remote(x_in.at[n], x_in.at[n], x_ss.at[n], x_rs.at[n], mate).wait_recv()
            total = mine + x_in[n].astype(F32)
            own[n] = total

            @pl.when(jnp.logical_and(me_z == 0, t > me_z))
            def _():
                z_out[n] = total.astype(BF16)
                hop(n, True).start()

            @pl.when(jnp.logical_and(me_z == z_n - 1, t < me_z))
            def _():
                z_out[n] = total.astype(BF16)
                hop(n, False).start()

    def relay_stage(which):
        for t in order:
            n = which * z_n + t

            @pl.when(jnp.logical_and(below, t > me_z))
            def _():
                hop(n, True).wait_recv()
                z_out[n] = (own[n] + up_in[n].astype(F32)).astype(BF16)
                hop(n, True).start()

            @pl.when(jnp.logical_and(above, t < me_z))
            def _():
                hop(n, False).wait_recv()
                z_out[n] = (own[n] + dn_in[n].astype(F32)).astype(BF16)
                hop(n, False).start()

    def gathered(which, put):
        for t in range(z_n):
            n = which * z_n + t

            @pl.when(t == me_z)
            def _():
                if t > 0:
                    hop(n, True).wait_recv()
                if t < z_n - 1:
                    hop(n, False).wait_recv()
                total = own[n]
                if t > 0:
                    total = total + up_in[n].astype(F32)
                if t < z_n - 1:
                    total = total + dn_in[n].astype(F32)
                put(total)

    def put_part(total):
        part[...] = total.astype(BF16).reshape(part.shape)

    def put_rows(total):
        rows_out[...] = total

    mate_stage(0)
    chip_stage(0)
    mate_stage(1)
    chip_stage(1)

    dw = depth // st_n
    for d in list(range(1, st_n)) + [0]:
        term = dot_tn(normed[:, rows_at(st_peer(d), dw)], dq_s[...])
        if d == 0:
            g_own[...] = term
        else:
            g_out[d] = term.astype(BF16)
            go(remote(
                g_out.at[d], g_in.at[d], g_ss.at[d], g_rs.at[d], (st_peer(d), me_tp)
            ))

    relay_stage(0)
    gathered(0, put_part)
    for s in range(st_n * slots):
        r_out[s] = part[req_of[s]]
    for d in range(1, st_n):
        go(remote(
            r_out.at[rows_at(st_peer(d), slots)], r_in.at[rows_at(me_st, slots)],
            r_ss.at[d], r_rs.at[d], (st_peer(d), me_tp),
        ))
    ret_out[rows_at(me_st, slots)] = r_out[rows_at(me_st, slots)]

    relay_stage(1)
    total = g_own[...]
    for d in range(1, st_n):
        remote(g_in.at[d], g_in.at[d], g_ss.at[d], g_rs.at[d], (st_peer(d), me_tp)).wait_recv()
        total = total + g_in[d].astype(F32)
    gqw_out[...] = total

    for d in range(1, st_n):
        span = rows_at(st_from(d), slots)
        remote(
            r_in.at[span], r_in.at[span], r_ss.at[d], r_rs.at[d], (st_peer(d), me_tp)
        ).wait_recv()
        ret_out[span] = r_in[span]

    gathered(1, put_rows)
    for copy in sends:
        copy.wait_send()
    for t in range(z_n):
        for which in range(2):

            @pl.when(t != me_z)
            def _():
                hop(which * z_n + t, True).wait_send()


def main_call(st_n, tp_n, reads, slot_of, req_of, served, normed, w_q, w_g, w_k, w_v, cot):
    tok, hw = cot.shape
    depth = w_q.shape[0]
    cw, dw, z_n = depth // tp_n, depth // st_n, tp_n // CORES
    ctx = tok // BLK * reads * PLEN
    slot_total = served.shape[0]
    vmem = pl.BlockSpec(memory_space=pltpu.VMEM)
    smem = pl.BlockSpec(memory_space=pltpu.SMEM)
    piece = lambda rows, n=2 * z_n: pltpu.VMEM((n, rows, cw), BF16)
    sem = lambda n: pltpu.SemaphoreType.DMA((n,))
    rows_most = max(ctx, tok)
    assert ctx == tok
    return pl.pallas_call(
        functools.partial(main_kernel, st_n, tp_n, reads),
        out_shape=(
            jax.ShapeDtypeStruct((tok, cw), F32),
            jax.ShapeDtypeStruct((slot_total, PLEN, cw), BF16),
            jax.ShapeDtypeStruct((dw, hw), F32),
        ),
        in_specs=[smem, smem] + [vmem] * 7,
        out_specs=(vmem, vmem, vmem),
        scratch_shapes=[
            pltpu.VMEM((slot_total, PLEN, 2 * hw), BF16),
            pltpu.VMEM((tok, hw), BF16),
            pltpu.VMEM((tok, hw), F32),
            pltpu.VMEM((tok, hw), BF16),
            pltpu.VMEM((tok, hw), BF16),
            pltpu.VMEM((ctx, 2 * hw), BF16),
            piece(rows_most), piece(rows_most), piece(rows_most), piece(rows_most), piece(rows_most),
            pltpu.VMEM((2 * z_n, rows_most, cw), F32),
            pltpu.VMEM((ctx // PLEN, PLEN, cw), BF16),
            pltpu.VMEM((slot_total, PLEN, cw), BF16),
            pltpu.VMEM((slot_total, PLEN, cw), BF16),
            pltpu.VMEM((st_n, dw, hw), BF16),
            pltpu.VMEM((st_n, dw, hw), BF16),
            pltpu.VMEM((dw, hw), F32),
            sem(st_n), sem(st_n), sem(2 * z_n), sem(2 * z_n), sem(2 * z_n), sem(2 * z_n), sem(2 * z_n),
            sem(st_n), sem(st_n), sem(st_n), sem(st_n),
        ],
        compiler_params=pltpu.CompilerParams(
            collective_id=0, has_side_effects=True, vmem_limit_bytes=56 << 20
        ),
        name="main",
    )(slot_of, req_of, served, normed, w_q, w_g, w_k, w_v, cot)


def spread_kernel(ids, returned, out_ref):
    out_ref[...] = jnp.zeros_like(out_ref)
    for s in range(ids.shape[0]):
        passage = ids[s]

        @pl.when(passage >= 0)
        def _():
            span = rows_at(passage, PLEN)
            out_ref[span, :] += returned[s].astype(F32)


def spread(ids, returned, rows):
    return pl.pallas_call(
        spread_kernel,
        out_shape=jax.ShapeDtypeStruct((rows, returned.shape[2]), F32),
        in_specs=[
            pl.BlockSpec(memory_space=pltpu.SMEM),
            pl.BlockSpec(memory_space=pltpu.VMEM),
        ],
        out_specs=pl.BlockSpec(memory_space=pltpu.VMEM),
        compiler_params=pltpu.CompilerParams(vmem_limit_bytes=16 << 20),
        name="spread",
    )(ids, returned)


def shards(normed, store, passage_ids, w_query, w_gate, w_key, w_value, cotangent):
    peer_count = lax.axis_size("st")
    blocks, read_count = passage_ids.shape
    requests = blocks * read_count
    slot_most = max(1, 2 * requests // peer_count)
    slot_count = peer_count * slot_most
    pass_dev = store.shape[0] // PLEN
    flat_ids = passage_ids.reshape(requests)
    owners = flat_ids // pass_dev
    local_ids = flat_ids % pass_dev
    positions = jnp.arange(requests, dtype=jnp.int32)
    before = (owners[:, None] == owners[None, :]) & (positions[None, :] < positions[:, None])
    slot_of = owners * slot_most + jnp.sum(before.astype(jnp.int32), axis=1)
    slot_hit = slot_of[:, None] == jnp.arange(slot_count, dtype=jnp.int32)[None, :]
    slot_table = jnp.max(jnp.where(slot_hit, local_ids[:, None], -1), axis=0)
    req_of = jnp.max(jnp.where(slot_hit, positions[:, None], 0), axis=0)
    served_ids = lax.all_to_all(
        slot_table.reshape(peer_count, slot_most), "st", split_axis=0, concat_axis=0, tiled=True
    ).reshape(slot_count)
    served = project(store, jnp.maximum(served_ids, 0), w_key, w_value)
    served = served.reshape(slot_count, PLEN, served.shape[1])
    grad_rows, returned, grad_query_weight = main_call(
        peer_count, lax.axis_size("tp"), read_count,
        slot_of, req_of, served, normed, w_query, w_gate, w_key, w_value, cotangent,
    )
    grad_store = spread(served_ids, returned, store.shape[0])
    return (grad_rows, grad_store, grad_query_weight)


def solution(mesh):
    placed = (
        P("st", None),
        P("st", None),
        P("st", None),
        P(None, "tp"),
        P(None, "tp"),
        P(None, "tp"),
        P(None, "tp"),
        P("st", "tp"),
    )
    return jax.shard_map(
        shards,
        mesh=mesh,
        in_specs=placed,
        out_specs=(P("st", "tp"), P("st", "tp"), P("st", "tp")),
        check_vma=False,
    )
```

```python
import functools

import jax
import jax.numpy as jnp
from jax import lax
from jax.experimental import pallas as pl
from jax.experimental.pallas import tpu as pltpu
from jax.sharding import PartitionSpec as P

DH = 128
BLK = 128
PLEN = 64
GROUP = 4
CORES = 2
F32 = jnp.float32
BF16 = jnp.bfloat16
MESH = pl.DeviceIdType.MESH


def dot_nn(a, b):
    return lax.dot_general(a, b, (((1,), (0,)), ((), ())), preferred_element_type=F32)


def dot_nt(a, b):
    return lax.dot_general(a, b, (((1,), (1,)), ((), ())), preferred_element_type=F32)


def dot_tn(a, b):
    return lax.dot_general(a, b, (((0,), (0,)), ((), ())), preferred_element_type=F32)


def rows_at(index, size):
    return pl.ds(pl.multiple_of(index * size, size), size)


def project_kernel(ids, *refs):
    passages = refs[:GROUP]
    wk_ref, wv_ref, out_ref = refs[GROUP:]
    rows = jnp.concatenate([p[...] for p in passages], axis=0)
    width = wk_ref.shape[1]
    out_ref[:, :width] = dot_nn(rows, wk_ref[...]).astype(BF16)
    out_ref[:, width:] = dot_nn(rows, wv_ref[...]).astype(BF16)


def project(store, ids, w_key, w_value):
    slots = ids.shape[0]
    depth, width = w_key.shape
    passage = lambda g: pl.BlockSpec((PLEN, depth), lambda i, ids: (ids[GROUP * i + g], 0))
    weight = pl.BlockSpec((depth, width), lambda i, ids: (0, 0))
    return pl.pallas_call(
        project_kernel,
        out_shape=jax.ShapeDtypeStruct((slots * PLEN, 2 * width), BF16),
        grid_spec=pltpu.PrefetchScalarGridSpec(
            num_scalar_prefetch=1,
            grid=(slots // GROUP,),
            in_specs=[passage(g) for g in range(GROUP)] + [weight, weight],
            out_specs=pl.BlockSpec((GROUP * PLEN, 2 * width), lambda i, ids: (i, 0)),
        ),
        compiler_params=pltpu.CompilerParams(vmem_limit_bytes=58 << 20),
        name="project",
    )(ids, *([store] * GROUP), w_key, w_value)


def main_kernel(
    st_n, tp_n, reads,
    slot_of, req_of, served, normed_h, w_q_h, w_g_h, w_k_h, w_v_h, cot_h,
    rows_out, ret_out, gqw_out,
    normed, w_q, w_g, w_k, w_v, cot, load_sem,
    arrived, q_s, gate_s, dq_s, dg_s, dp_s,
    x_out, x_in, z_out, up_in, dn_in, own, part, r_out, r_in, g_out, g_in, g_own,
    kv_ss, kv_rs, x_ss, x_rs, z_ss, up_rs, dn_rs, r_ss, r_rs, g_ss, g_rs,
):
    me_st, me_tp = lax.axis_index("st"), lax.axis_index("tp")
    z_n = tp_n // CORES
    me_z, me_c = me_tp // CORES, me_tp % CORES
    mate = (me_st, me_z * CORES + 1 - me_c)
    tok, hw = cot.shape
    depth = w_q.shape[0]
    heads = hw // DH
    blocks = tok // BLK
    cw = depth // tp_n
    slots = served.shape[0] // st_n
    scale = DH ** (-0.5)

    def st_peer(d):
        return lax.rem(me_st + d, st_n)

    def st_from(d):
        return lax.rem(me_st + st_n - d, st_n)

    def z_peer(d):
        return lax.rem(me_z + d, z_n)

    loads = []
    pairs = ((normed_h, normed), (w_q_h, w_q), (w_g_h, w_g), (cot_h, cot), (w_k_h, w_k), (w_v_h, w_v))
    for i, (far, near) in enumerate(pairs):
        loads.append(pltpu.make_async_copy(far, near, load_sem.at[i]))
        loads[-1].start()

    barrier = pltpu.get_barrier_semaphore()
    for d in range(1, st_n):
        pl.semaphore_signal(barrier, inc=1, device_id=(st_peer(d), me_tp), device_id_type=MESH)
    for d in range(1, z_n):
        pl.semaphore_signal(
            barrier, inc=1, device_id=(me_st, z_peer(d) * CORES + me_c), device_id_type=MESH
        )
    pl.semaphore_signal(barrier, inc=1, device_id=mate, device_id_type=MESH)
    pl.semaphore_wait(barrier, st_n + z_n - 1)

    def remote(src, dst, ss, rs, dev):
        return pltpu.make_async_remote_copy(
            src_ref=src, dst_ref=dst, send_sem=ss, recv_sem=rs, device_id=dev, device_id_type=MESH
        )

    sends = []

    def go(copy):
        copy.start()
        sends.append(copy)

    for d in range(1, st_n):
        go(remote(
            served.at[rows_at(st_peer(d), slots)], arrived.at[rows_at(me_st, slots)],
            kv_ss.at[d], kv_rs.at[d], (st_peer(d), me_tp),
        ))
    arrived[rows_at(me_st, slots)] = served[rows_at(me_st, slots)]

    for load in loads:
        load.wait()
    tile = 2 * BLK

    @pl.loop(0, tok // tile)
    def _(i):
        span = rows_at(i, tile)
        q_s[span, :] = dot_nn(normed[span, :], w_q[...]).astype(BF16)
        gate_s[span, :] = jax.nn.sigmoid(dot_nn(normed[span, :], w_g[...]))

    for d in range(1, st_n):
        here = arrived.at[rows_at(st_from(d), slots)]
        remote(here, here, kv_ss.at[d], kv_rs.at[d], (st_peer(d), me_tp)).wait_recv()

    for b in range(blocks):
        kv = jnp.concatenate(
            [arrived[slot_of[b * reads + r]] for r in range(reads)], axis=0
        )
        toks = slice(b * BLK, (b + 1) * BLK)
        span = reads * PLEN
        ctx = slice(b * span, (b + 1) * span)
        for h in range(heads):
            ch = slice(h * DH, (h + 1) * DH)
            chv = slice(hw + h * DH, hw + (h + 1) * DH)
            k, v = kv[:, ch], kv[:, chv]
            q = q_s[toks, ch]
            gate = gate_s[toks, ch]
            up = cot[toks, ch].astype(F32)
            s = dot_nt(q, k) * scale
            e = jnp.exp(s - jnp.max(s, axis=1, keepdims=True))
            p = e / jnp.sum(e, axis=1, keepdims=True)
            low = p.astype(BF16)
            att = dot_nn(low, v)
            d_att = (up * gate).astype(BF16)
            dg_s[toks, ch] = (up * att * gate * (1.0 - gate)).astype(BF16)
            dp_s[ctx, chv] = dot_tn(low, d_att).astype(BF16)
            d_p = dot_nt(d_att, v)
            delta = jnp.sum(d_p * p, axis=1, keepdims=True)
            d_s = (p * (d_p - delta) * scale).astype(BF16)
            dq_s[toks, ch] = dot_nn(d_s, k).astype(BF16)
            dp_s[ctx, ch] = dot_tn(d_s, q).astype(BF16)

    def chunk(which, t):
        w_rows = rows_at(t, cw)
        if which == 0:
            return dot_nt(dp_s[:, :hw], w_k[w_rows, :]) + dot_nt(dp_s[:, hw:], w_v[w_rows, :])
        return dot_nt(dq_s[...], w_q[w_rows, :]) + dot_nt(dg_s[...], w_g[w_rows, :])

    order = []
    for i in range((z_n + 1) // 2):
        order += [z_n - 1 - i, i] if z_n - 1 - i != i else [i]
    above, below = me_z < z_n - 1, me_z > 0

    def mate_stage(which, t):
        n = which * z_n + t
        x_out[n] = chunk(which, t * CORES + 1 - me_c).astype(BF16)
        go(remote(x_out.at[n], x_in.at[n], x_ss.at[n], x_rs.at[n], mate))

    def hop(n, up):
        landing, rs = (up_in, up_rs) if up else (dn_in, dn_rs)
        to = me_z + 1 if up else me_z - 1
        return remote(
            z_out.at[n], landing.at[n], z_ss.at[n], rs.at[n], (me_st, to * CORES + me_c)
        )

    def chip_stage(which, t):
        if True:
            n = which * z_n + t
            mine = chunk(which, t * CORES + me_c)
            remote(x_in.at[n], x_in.at[n], x_ss.at[n], x_rs.at[n], mate).wait_recv()
            total = mine + x_in[n].astype(F32)
            own[n] = total

            @pl.when(jnp.logical_and(me_z == 0, t > me_z))
            def _():
                z_out[n] = total.astype(BF16)
                hop(n, True).start()

            @pl.when(jnp.logical_and(me_z == z_n - 1, t < me_z))
            def _():
                z_out[n] = total.astype(BF16)
                hop(n, False).start()

    def relay_stage(which):
        for t in order:
            n = which * z_n + t

            @pl.when(jnp.logical_and(below, t > me_z))
            def _():
                hop(n, True).wait_recv()
                z_out[n] = (own[n] + up_in[n].astype(F32)).astype(BF16)
                hop(n, True).start()

            @pl.when(jnp.logical_and(above, t < me_z))
            def _():
                hop(n, False).wait_recv()
                z_out[n] = (own[n] + dn_in[n].astype(F32)).astype(BF16)
                hop(n, False).start()

    def gathered(which, put):
        for t in range(z_n):
            n = which * z_n + t

            @pl.when(t == me_z)
            def _():
                if t > 0:
                    hop(n, True).wait_recv()
                if t < z_n - 1:
                    hop(n, False).wait_recv()
                total = own[n]
                if t > 0:
                    total = total + up_in[n].astype(F32)
                if t < z_n - 1:
                    total = total + dn_in[n].astype(F32)
                put(total)

    def put_part(total):
        part[...] = total.astype(BF16).reshape(part.shape)

    def put_rows(total):
        rows_out[...] = total

    ahead = 2
    queue = [(which, t) for which in range(2) for t in order]
    for i in range(len(queue) + ahead):
        if i < len(queue):
            mate_stage(*queue[i])
        if i >= ahead:
            chip_stage(*queue[i - ahead])

    dw = depth // st_n
    for d in list(range(1, st_n)) + [0]:
        term = dot_tn(normed[:, rows_at(st_peer(d), dw)], dq_s[...])
        if d == 0:
            g_own[...] = term
        else:
            g_out[d] = term.astype(BF16)
            go(remote(
                g_out.at[d], g_in.at[d], g_ss.at[d], g_rs.at[d], (st_peer(d), me_tp)
            ))

    relay_stage(0)
    gathered(0, put_part)
    for s in range(st_n * slots):
        r_out[s] = part[req_of[s]]
    for d in range(1, st_n):
        go(remote(
            r_out.at[rows_at(st_peer(d), slots)], r_in.at[rows_at(me_st, slots)],
            r_ss.at[d], r_rs.at[d], (st_peer(d), me_tp),
        ))
    ret_out[rows_at(me_st, slots)] = r_out[rows_at(me_st, slots)]

    relay_stage(1)
    total = g_own[...]
    for d in range(1, st_n):
        remote(g_in.at[d], g_in.at[d], g_ss.at[d], g_rs.at[d], (st_peer(d), me_tp)).wait_recv()
        total = total + g_in[d].astype(F32)
    gqw_out[...] = total

    for d in range(1, st_n):
        span = rows_at(st_from(d), slots)
        remote(
            r_in.at[span], r_in.at[span], r_ss.at[d], r_rs.at[d], (st_peer(d), me_tp)
        ).wait_recv()
        ret_out[span] = r_in[span]

    gathered(1, put_rows)
    for copy in sends:
        copy.wait_send()
    for t in range(z_n):
        for which in range(2):

            @pl.when(t != me_z)
            def _():
                hop(which * z_n + t, True).wait_send()


def main_call(st_n, tp_n, reads, slot_of, req_of, served, normed, w_q, w_g, w_k, w_v, cot):
    tok, hw = cot.shape
    depth = w_q.shape[0]
    cw, dw, z_n = depth // tp_n, depth // st_n, tp_n // CORES
    ctx = tok // BLK * reads * PLEN
    slot_total = served.shape[0]
    vmem = pl.BlockSpec(memory_space=pltpu.VMEM)
    smem = pl.BlockSpec(memory_space=pltpu.SMEM)
    piece = lambda rows, n=2 * z_n: pltpu.VMEM((n, rows, cw), BF16)
    sem = lambda n: pltpu.SemaphoreType.DMA((n,))
    rows_most = max(ctx, tok)
    assert ctx == tok
    return pl.pallas_call(
        functools.partial(main_kernel, st_n, tp_n, reads),
        out_shape=(
            jax.ShapeDtypeStruct((tok, cw), F32),
            jax.ShapeDtypeStruct((slot_total, PLEN, cw), BF16),
            jax.ShapeDtypeStruct((dw, hw), F32),
        ),
        in_specs=[smem, smem, vmem] + [pl.BlockSpec(memory_space=pl.ANY)] * 6,
        out_specs=(vmem, vmem, vmem),
        scratch_shapes=[
            *[pltpu.VMEM(a.shape, a.dtype) for a in (normed, w_q, w_g, w_k, w_v, cot)],
            sem(6),
            pltpu.VMEM((slot_total, PLEN, 2 * hw), BF16),
            pltpu.VMEM((tok, hw), BF16),
            pltpu.VMEM((tok, hw), F32),
            pltpu.VMEM((tok, hw), BF16),
            pltpu.VMEM((tok, hw), BF16),
            pltpu.VMEM((ctx, 2 * hw), BF16),
            piece(rows_most), piece(rows_most), piece(rows_most), piece(rows_most), piece(rows_most),
            pltpu.VMEM((2 * z_n, rows_most, cw), F32),
            pltpu.VMEM((ctx // PLEN, PLEN, cw), BF16),
            pltpu.VMEM((slot_total, PLEN, cw), BF16),
            pltpu.VMEM((slot_total, PLEN, cw), BF16),
            pltpu.VMEM((st_n, dw, hw), BF16),
            pltpu.VMEM((st_n, dw, hw), BF16),
            pltpu.VMEM((dw, hw), F32),
            sem(st_n), sem(st_n), sem(2 * z_n), sem(2 * z_n), sem(2 * z_n), sem(2 * z_n), sem(2 * z_n),
            sem(st_n), sem(st_n), sem(st_n), sem(st_n),
        ],
        compiler_params=pltpu.CompilerParams(
            collective_id=0, has_side_effects=True, vmem_limit_bytes=56 << 20
        ),
        name="main",
    )(slot_of, req_of, served, normed, w_q, w_g, w_k, w_v, cot)


def spread_kernel(ids, returned, rows, gqw, out_ref, rows_ref, gqw_ref):
    rows_ref[...] = rows[...]
    gqw_ref[...] = gqw[...]
    out_ref[...] = jnp.zeros_like(out_ref)
    for s in range(ids.shape[0]):
        passage = ids[s]

        @pl.when(passage >= 0)
        def _():
            span = rows_at(passage, PLEN)
            out_ref[span, :] += returned[s].astype(F32)


def spread(ids, returned, grad_rows, grad_query_weight, rows):
    vmem = pl.BlockSpec(memory_space=pltpu.VMEM)
    return pl.pallas_call(
        spread_kernel,
        out_shape=(
            jax.ShapeDtypeStruct((rows, returned.shape[2]), F32),
            jax.ShapeDtypeStruct(grad_rows.shape, F32),
            jax.ShapeDtypeStruct(grad_query_weight.shape, F32),
        ),
        in_specs=[pl.BlockSpec(memory_space=pltpu.SMEM), vmem, vmem, vmem],
        out_specs=(vmem, vmem, vmem),
        compiler_params=pltpu.CompilerParams(vmem_limit_bytes=60 << 20),
        name="spread",
    )(ids, returned, grad_rows, grad_query_weight)


def shards(normed, store, passage_ids, w_query, w_gate, w_key, w_value, cotangent):
    peer_count = lax.axis_size("st")
    blocks, read_count = passage_ids.shape
    requests = blocks * read_count
    slot_most = max(1, 2 * requests // peer_count)
    slot_count = peer_count * slot_most
    pass_dev = store.shape[0] // PLEN
    flat_ids = passage_ids.reshape(requests)
    owners = flat_ids // pass_dev
    local_ids = flat_ids % pass_dev
    positions = jnp.arange(requests, dtype=jnp.int32)
    before = (owners[:, None] == owners[None, :]) & (positions[None, :] < positions[:, None])
    slot_of = owners * slot_most + jnp.sum(before.astype(jnp.int32), axis=1)
    slot_hit = slot_of[:, None] == jnp.arange(slot_count, dtype=jnp.int32)[None, :]
    slot_table = jnp.max(jnp.where(slot_hit, local_ids[:, None], -1), axis=0)
    req_of = jnp.max(jnp.where(slot_hit, positions[:, None], 0), axis=0)
    served_ids = lax.all_to_all(
        slot_table.reshape(peer_count, slot_most), "st", split_axis=0, concat_axis=0, tiled=True
    ).reshape(slot_count)
    served = project(store, jnp.maximum(served_ids, 0), w_key, w_value)
    served = served.reshape(slot_count, PLEN, served.shape[1])
    grad_rows, returned, grad_query_weight = main_call(
        peer_count, lax.axis_size("tp"), read_count,
        slot_of, req_of, served, normed, w_query, w_gate, w_key, w_value, cotangent,
    )
    grad_store, grad_rows, grad_query_weight = spread(
        served_ids, returned, grad_rows, grad_query_weight, store.shape[0]
    )
    return (grad_rows, grad_store, grad_query_weight)


def solution(mesh):
    placed = (
        P("st", None),
        P("st", None),
        P("st", None),
        P(None, "tp"),
        P(None, "tp"),
        P(None, "tp"),
        P(None, "tp"),
        P("st", "tp"),
    )
    return jax.shard_map(
        shards,
        mesh=mesh,
        in_specs=placed,
        out_specs=(P("st", "tp"), P("st", "tp"), P("st", "tp")),
        check_vma=False,
    )
```
